32 devices in a mesh: grp: 2 (over y), fs: 4 (over z), tp: 4 (over x, core).
Axes of the slice: x: 2, y: 2, z: 4, core: 2. Of those that a mesh axis runs over, the one named last changes fastest.
Arguments:
- tokens: bfloat16 [3072, 4096], P(('grp', 'fs'), 'tp'), parts along dimension 0, may hold values from -1100 to 1100
- norm_gain: float32 [4096], P('fs'), may hold values from 0.1 to 1.9
- gate_master: float32 [4, 4096, 512], P(None, 'fs', 'tp'), may hold values from -0.09375 to 0.09375
- up_master: float32 [4, 4096, 512], P(None, 'fs', 'tp'), may hold values from -0.09375 to 0.09375
- down_master: float32 [4, 512, 4096], P(None, 'fs', 'tp'), may hold values from -0.25 to 0.25
- expert_ids: int32 [3072, 2], P(('grp', 'fs')), parts along dimension 0, may hold values from 0 to 3, as said below
- route_weights: float32 [3072, 2], P(('grp', 'fs')), parts along dimension 0, may hold values from 0.2 to 1
Outputs:
- gate_sampler: bfloat16 [8, 4096, 512], P(('grp', 'fs'), None, 'tp'), parts along dimension 0
- up_sampler: bfloat16 [8, 4096, 512], P(('grp', 'fs'), None, 'tp'), parts along dimension 0
- down_sampler: bfloat16 [8, 512, 4096], P(('grp', 'fs'), 'tp'), parts along dimension 0
- mixed: bfloat16 [3072, 4096], P(('grp', 'fs'), 'tp'), parts along dimension 0
The draws below stay inside these ranges and needn't reach their ends.
There are 2 independent parts, one for each index of `grp`. The reference program is written for one: setup_inputs(seed, part) draws one part's arguments, and reference() takes and returns one part's arrays. A program takes and returns all parts, laid end to end along the dimension named above; an argument that names none is the same for every part. Nothing has to cross between parts.
Inputs may be any that keep to these rules, and one draw needn't show every extreme that they name: `expert_ids`: each row names two different experts of one group: experts g * 2 to (g + 1) * 2 - 1 for some g. In each aligned block of 384 rows every expert is named exactly 192 times.
All inputs are finite; a program needn't handle non-finite values.
Results may differ from the reference program's by a relative error of at most 0.0091.
Values may be sent and summed in bfloat16 or wider, within the bound.
No kernel may reach another device: no remote copies, remote signals or barrier semaphores. Data moves between devices by JAX's collectives and lax.ppermute only.
A program may use at most 128 MiB of HBM per device.

```python
import math
import jax
import jax.numpy as jnp
from jax import lax

D = 4096
FF = 512
TOP = 2
TOK_DEV = 384
EXPERTS = 4
GROUPS = 2
TOKENS = 1536
N_TP = 4


def draw_tokens(key, part):
    k_base, k_column, k_row = jax.random.split(jax.random.fold_in(key, 3), 3)
    column = jnp.arange(D, dtype=jnp.float32) / D
    column_scale = 10.0 ** column * jnp.exp(jax.random.uniform(k_column, (D,), jnp.float32, -0.7, 0.7))
    row_scale = jnp.exp(jax.random.uniform(k_row, (TOKENS, 1), jnp.float32, 0.0, math.log(10.0)))
    base = jax.random.normal(k_base, (TOKENS, D), jnp.float32)
    base = jnp.clip(base, -5.0, 5.0)
    return (base * column_scale[None, :] * row_scale).astype(jnp.bfloat16)


def draw_expert_ids(key, part):
    blocks = TOKENS // TOK_DEV
    per_group = EXPERTS // GROUPS
    keys = jax.random.split(jax.random.fold_in(key, 11), blocks)

    def one_block(block_key):
        k_rank, k_turn = jax.random.split(block_key)
        rank = jax.random.permutation(k_rank, TOK_DEV).astype(jnp.int32)
        group = rank % GROUPS
        within = rank // GROUPS
        turn = jax.random.randint(k_turn, (GROUPS,), 0, per_group).astype(jnp.int32)
        first = (within + turn[group]) % per_group
        stride = 1 + within // per_group % (per_group - 1)
        second = (first + stride) % per_group
        return jnp.stack([group * per_group + first, group * per_group + second], axis=1)
    return jax.vmap(one_block)(keys).reshape(TOKENS, TOP).astype(jnp.int32)


def block_levels(key, shape, cuts, low, top_value):
    def one(axis_at, blocks):
        heights = jax.random.uniform(jax.random.fold_in(jax.random.fold_in(key, 6), axis_at), (blocks,), jnp.float32, low / len(cuts), top_value / len(cuts))
        return jnp.repeat(jnp.exp(heights), shape[axis_at] // blocks).reshape((-1,) + (1,) * (len(shape) - axis_at - 1))

    level = one(*cuts[0])
    for cut in cuts[1:]:
        level = level * one(*cut)
    return level


def bell_draw(own_key, shape, width, reach, cuts=(), kind=jnp.bfloat16):
    result = width * jax.random.normal(own_key, shape, jnp.float32)
    if cuts:
        result = result * block_levels(own_key, shape, cuts, -0.22, 0.18)
    return jnp.clip(result, -reach, reach).astype(kind)


def setup_inputs(seed: int = 0, part: int = 0) -> dict:
    seeds = jax.random.split(jax.random.key(seed), 8)
    part_splits = jax.random.split(jax.random.fold_in(seeds[7], part), 8)
    return {
        "tokens": draw_tokens(jax.random.fold_in(jax.random.fold_in(seeds[7], part), 71), part),
        "norm_gain": jnp.clip(1.0 + 0.18 * jax.random.normal(seeds[1], (D,), jnp.float32), 0.1, 1.9),
        "gate_master": bell_draw(seeds[2], (EXPERTS, D, FF), D ** -0.5, 0.09375, ((1, 4), (2, 4)), jnp.float32),
        "up_master": bell_draw(seeds[3], (EXPERTS, D, FF), D ** -0.5, 0.09375, ((1, 4), (2, 4)), jnp.float32),
        "down_master": bell_draw(seeds[4], (EXPERTS, FF, D), FF ** -0.5, 0.25, ((1, 4), (2, 4)), jnp.float32),
        "expert_ids": draw_expert_ids(jax.random.fold_in(jax.random.fold_in(seeds[7], part), 71), part),
        "route_weights": jnp.clip(jnp.exp(math.log(1.0) - 1.609438 * jax.random.uniform(part_splits[6], (TOKENS, TOP), jnp.float32) ** block_levels(part_splits[6], (TOKENS, TOP), ((0, 4),), -0.2, 0.2)), 0.2, 1.0),
    }


def reference(tokens, norm_gain, gate_master, up_master, down_master, expert_ids, route_weights):
    gate_w = (norm_gain[None, :, None] * gate_master).astype(jnp.bfloat16)
    up_w = (norm_gain[None, :, None] * up_master).astype(jnp.bfloat16)
    down_w = down_master.astype(jnp.bfloat16)
    values = tokens.astype(jnp.float32)
    normed = (values * lax.rsqrt(lax.optimization_barrier(jnp.mean(values * values, axis=1, keepdims=True)) + 1e-06)).astype(jnp.bfloat16)
    flat = expert_ids.reshape(-1)
    order = jnp.argsort(flat, stable=True).astype(jnp.int32)
    per_expert = flat.shape[0] // EXPERTS
    owners = (order // TOP).astype(jnp.int32).reshape(EXPERTS, per_expert)
    weights = route_weights.reshape(-1)[order].reshape(EXPERTS, per_expert)
    block = FF // N_TP

    def run_expert(inputs):
        e_gate, e_up, e_down, rows = inputs
        picked = normed[rows]
        gate = jnp.dot(picked, e_gate, preferred_element_type=jnp.float32)
        up = jnp.dot(picked, e_up, preferred_element_type=jnp.float32)
        hidden = (jax.nn.silu(gate) * up).astype(jnp.bfloat16)
        total = jnp.zeros((picked.shape[0], D), jnp.float32)
        for index in range(N_TP):
            partial_value = jnp.dot(hidden[:, index * block:(index + 1) * block], e_down[index * block:(index + 1) * block], preferred_element_type=jnp.float32).astype(jnp.bfloat16)
            total = total + lax.optimization_barrier(partial_value).astype(jnp.float32)
        return total.astype(jnp.bfloat16)
    outputs = lax.map(run_expert, (gate_w, up_w, down_w, owners))
    weighted = outputs.astype(jnp.float32) * weights[:, :, None]
    mixed = jnp.zeros((tokens.shape[0], D), jnp.float32).at[owners.reshape(-1)].add(weighted.reshape(-1, D))
    return (gate_w, up_w, down_w, mixed.astype(jnp.bfloat16))
```

```python
import functools

import jax
import jax.numpy as jnp
from jax import lax
from jax.experimental import pallas as pl
from jax.experimental.pallas import tpu as pltpu
from jax.sharding import PartitionSpec as P


F32 = jnp.float32
BF16 = jnp.bfloat16


def vmem(count):
    return [pl.BlockSpec(memory_space=pltpu.VMEM)] * count


def smem():
    return pl.BlockSpec(memory_space=pltpu.SMEM)


def call(body, outs, ins, flops, name):
    size = sum(a.size * a.dtype.itemsize for a in ins)
    size += sum(o.size * o.dtype.itemsize for o in outs)
    return pl.pallas_call(
        body,
        out_shape=outs,
        in_specs=[smem()] + vmem(len(ins) - 1),
        out_specs=vmem(len(outs)),
        cost_estimate=pl.CostEstimate(
            flops=flops, bytes_accessed=size, transcendentals=0
        ),
        compiler_params=pltpu.CompilerParams(vmem_limit_bytes=40 << 20),
        name=name,
    )(*ins)


def shape(dims, dtype=BF16):
    return jax.ShapeDtypeStruct(tuple(dims), dtype)


def shift(x, axis, step):
    n = lax.axis_size(axis)
    return lax.ppermute(x, axis, [(i, (i + step) % n) for i in range(n)])


def hop(x, axis, step):
    n = lax.axis_size(axis)
    return lax.ppermute(
        x, axis, [(i, i + step) for i in range(n) if 0 <= i + step < n]
    )


def slot_table(ids, first, experts):
    count = ids.shape[0]
    lanes = lax.broadcasted_iota(jnp.int32, (count, 128), 1)
    wanted = lax.rem(lanes + first, experts)
    named = jnp.zeros((count, 128), jnp.bool_)
    for k in range(ids.shape[1]):
        named = named | (ids[:, k : k + 1] == wanted)
    marks = jnp.where(named, 1.0, 0.0).astype(BF16)
    rows = lax.broadcasted_iota(jnp.int32, (count, count), 0)
    cols = lax.broadcasted_iota(jnp.int32, (count, count), 1)
    lower = jnp.where(rows >= cols, 1.0, 0.0).astype(BF16)
    upto = jnp.dot(lower, marks, preferred_element_type=F32)
    return jnp.where(named, upto - 1.0, -1.0)


def selection(places, capacity):
    slots = lax.broadcasted_iota(jnp.int32, (places.shape[0], capacity), 1)
    return jnp.where(places.astype(jnp.int32) == slots, 1.0, 0.0).astype(BF16)


def dispatch_body(experts, pos, tok, scale, ids, *outs):
    places = slot_table(ids[...], pos[0], experts)
    normed = (tok[...].astype(F32) * scale[...]).astype(BF16)
    for s in range(experts):
        chosen = selection(places[:, s : s + 1], outs[s].shape[0])
        outs[s][...] = lax.dot_general(
            chosen, normed, (((0,), (0,)), ((), ())), preferred_element_type=F32
        ).astype(BF16)


def place_body(n, pos, local, near, far, whole, *sends):
    f, t, g = pos[0], pos[1], pos[2]
    rows = near.shape[1]

    def put(block, half, value):
        start = pl.multiple_of((block * 2 + half) * rows, rows)
        whole[pl.ds(start, rows), :] = value

    for half in range(2):
        put(f, half, local[half])
    for s in range(1, n):
        block = lax.rem(f - s + n, n)
        put(block, g, near[s - 1])
        put(block, 1 - g, far[s - 1])
    for u in range(n):
        start = pl.multiple_of(lax.rem(t + u, n) * 2 * rows, 2 * rows)
        sends[u][...] = whole[pl.ds(start, 2 * rows), :]


def preact_body(n, pos, *refs):
    xs, gate, up, out = refs[:n], refs[n], refs[n + 1], refs[n + 2]
    both = jnp.concatenate([gate[...], up[...]], axis=1)
    for s in range(n):
        out[s] = jnp.dot(xs[s][...], both, preferred_element_type=F32).astype(out.dtype)


def hidden_body(n, pos, *refs):
    parts, outs = refs[:n], refs[n:]
    width = outs[0].shape[1]
    for s in range(n):
        total = parts[0][s].astype(F32)
        for part in parts[1:]:
            total = total + part[s].astype(F32)
        gate, up = total[:, :width], total[:, width:]
        outs[s][...] = (gate / (1.0 + jnp.exp(-gate)) * up).astype(BF16)


def mix_body(n, pos, ids, weights, hid, *refs):
    near, far, out = refs[:n], refs[n : 2 * n], refs[2 * n]
    f, g = pos[0], pos[2]
    count, top = ids.shape
    per_half = near[0].shape[0]
    capacity = hid.shape[2]
    id_values = ids[...]
    w_values = weights[...]
    total = jnp.zeros(out.shape, F32)
    for refs_of, owner in ((near, g), (far, 1 - g)):
        places = slot_table(id_values, owner * per_half, n)
        for j in range(per_half):
            expert = owner * per_half + j
            s = lax.rem(expert - f + n, n)
            chosen = selection(places[:, j : j + 1], capacity)
            weight = jnp.zeros((count, 1), F32)
            for k in range(top):
                weight = weight + jnp.where(
                    id_values[:, k : k + 1] == expert, w_values[:, k : k + 1], 0.0
                )
            rows = []
            blocks = []
            for k in range(n):
                block = lax.rem(f - k + n, n)
                picked = jnp.dot(chosen, hid[block, s], preferred_element_type=F32)
                rows.append((picked * weight).astype(BF16))
                blocks.append(refs_of[k][j])
            total = total + jnp.dot(
                jnp.concatenate(rows, axis=1),
                jnp.concatenate(blocks, axis=0),
                preferred_element_type=F32,
            )
    out[...] = total.astype(BF16)


def pick_body(n, pos, *refs):
    blocks, outs, sem = refs[: 2 * n], refs[2 * n : 3 * n], refs[3 * n]
    f, t, g = pos[0], pos[1], pos[2]
    per_half = blocks[0].shape[0]
    owner = lax.div(f, per_half)
    index = lax.rem(f, per_half)
    for u in range(n):
        k = lax.rem(f - t - u + 2 * n, n)
        for side in range(2):
            for kk in range(n):
                mine = (k == kk) & ((owner == g) if side == 0 else (owner != g))

                @pl.when(mine)
                def _(u=u, side=side, kk=kk):
                    copy = pltpu.make_async_copy(
                        blocks[side * n + kk].at[index], outs[u], sem.at[u]
                    )
                    copy.start()
                    copy.wait()


def join_body(n, pos, *refs):
    parts, out = refs[:n], refs[n]
    width = parts[0].shape[1]
    for u in range(n):
        start = pl.multiple_of(lax.rem(pos[1] - u + n, n) * width, width)
        out[:, pl.ds(start, width)] = parts[u][...]


def quick(tokens, norm_gain, gate_master, up_master, down_master, expert_ids, route_weights):
    n = lax.axis_size("fs")
    f, t, g = lax.axis_index("fs"), lax.axis_index("tp"), lax.axis_index("grp")
    pos = jnp.stack([f, t, g]).astype(jnp.int32)
    count, width = tokens.shape
    capacity = expert_ids.shape[1] * count // n
    rows, ff = gate_master.shape[1], gate_master.shape[2]
    half = rows // 2
    per_half = n // 2

    def half_of(master, expert, which):
        part = lax.dynamic_slice(master, (expert, which * half, 0), (1, half, ff))[0]
        gain = lax.dynamic_slice(norm_gain, (which * half,), (half,))
        return (part * gain[:, None]).astype(BF16)

    def along_fs(master):
        return [
            shift(half_of(master, (f + s) % n, g), "fs", s) for s in range(1, n)
        ]

    gate_near = along_fs(gate_master)
    up_near = along_fs(up_master)

    values = tokens.astype(F32)
    squares = lax.psum(jnp.sum(values * values, axis=1), "tp")
    scale = lax.rsqrt(squares / (width * lax.axis_size("tp")) + 1e-06)[:, None]
    xs = call(
        functools.partial(dispatch_body, n),
        [shape((capacity, width))] * n,
        [pos, tokens, scale, expert_ids],
        2 * n * count * capacity * width,
        "dispatch",
    )
    xs = [xs[0]] + [shift(xs[s], "fs", s) for s in range(1, n)]

    def settle(near, master, name):
        near = jnp.stack(near)
        far = shift(near, "grp", 1)
        local = (
            lax.dynamic_index_in_dim(master, f, 0, keepdims=False) * norm_gain[:, None]
        ).astype(BF16)
        out = call(
            functools.partial(place_body, n),
            [shape((n * rows, ff))] + [shape((rows, ff))] * n,
            [pos, local.reshape(2, half, ff), near, far],
            n * rows * ff,
            name,
        )
        whole, sends = out[0], out[1:]
        blocks = [sends[0]] + [shift(sends[u], "tp", u) for u in range(1, n)]
        return whole, blocks

    gate_whole, gate_blocks = settle(gate_near, gate_master, "gate_rows")
    up_whole, up_blocks = settle(up_near, up_master, "up_rows")

    down = down_master.astype(BF16)
    own = lax.dynamic_slice(
        down, (g * per_half, 0, 0), (per_half,) + down.shape[1:]
    )
    other = lax.dynamic_slice(
        down, ((1 - g) * per_half, 0, 0), (per_half,) + down.shape[1:]
    )
    rights, lefts = [own], [own]
    for _ in range(1, n):
        rights.append(hop(rights[-1], "fs", 1))
        lefts.append(hop(lefts[-1], "fs", -1))
    near = [own] + [jnp.where(f >= k, rights[k], lefts[n - k]) for k in range(1, n)]
    far = [other] + [shift(near[k], "grp", 1) for k in range(1, n)]

    parts = []
    for u in range(n):
        parts.append(
            call(
                functools.partial(preact_body, n),
                [shape((n, capacity, 2 * ff), F32 if u == 0 else BF16)],
                [pos] + xs + [gate_blocks[u], up_blocks[u]],
                2 * n * capacity * rows * 2 * ff,
                "preact",
            )[0]
        )
    parts = [parts[0]] + [shift(parts[u], "tp", -u) for u in range(1, n)]
    hidden = call(
        functools.partial(hidden_body, n),
        [shape((capacity, ff))] * n,
        [pos] + parts,
        10 * n * capacity * ff,
        "hidden",
    )
    hidden = [hidden[0]] + [shift(hidden[s], "fs", -s) for s in range(1, n)]
    hidden = lax.all_gather(jnp.stack(hidden), "tp")

    mixed = call(
        functools.partial(mix_body, n),
        [shape((count, width))],
        [pos, expert_ids, route_weights, hidden] + near + far,
        2 * n * count * (capacity + width) * n * ff,
        "mix",
    )[0]

    picked = pl.pallas_call(
        functools.partial(pick_body, n),
        out_shape=[shape(down.shape[1:])] * n,
        in_specs=[smem()] + [pl.BlockSpec(memory_space=pl.ANY)] * (2 * n),
        out_specs=vmem(n),
        scratch_shapes=[pltpu.SemaphoreType.DMA((n,))],
        cost_estimate=pl.CostEstimate(
            flops=down.size, bytes_accessed=4 * down.size, transcendentals=0
        ),
        name="pick",
    )(pos, *near, *far)
    picked = [picked[0]] + [shift(picked[u], "tp", u) for u in range(1, n)]
    down_whole = call(
        functools.partial(join_body, n),
        [shape((down.shape[1], n * width))],
        [pos] + picked,
        down.size,
        "down_rows",
    )[0]
    return gate_whole[None], up_whole[None], down_whole[None], mixed


def plain(tokens, norm_gain, gate_master, up_master, down_master, expert_ids, route_weights):
    gain = norm_gain[None, :, None]
    gate_new = (gain * gate_master).astype(jnp.bfloat16)
    up_new = (gain * up_master).astype(jnp.bfloat16)
    gate_local, up_local = (
        lax.all_to_all(gate_new, "fs", split_axis=0, concat_axis=1, tiled=True),
        lax.all_to_all(up_new, "fs", split_axis=0, concat_axis=1, tiled=True),
    )
    down_local = lax.all_to_all(
        lax.all_to_all(
            down_master.astype(jnp.bfloat16), "fs", split_axis=0, concat_axis=1, tiled=True
        ),
        "tp",
        split_axis=1,
        concat_axis=2,
        tiled=True,
    )
    experts = lax.axis_size("fs")
    count = expert_ids.shape[0]
    top = expert_ids.shape[1]
    capacity = top * count // experts
    flat = expert_ids.reshape(-1)
    onehot = (flat[:, None] == jnp.arange(experts, dtype=jnp.int32)[None, :]).astype(jnp.int32)
    place = jnp.sum(jnp.cumsum(onehot, axis=0) * onehot, axis=1) - 1
    slots = flat * capacity + place
    owners = (
        jnp.zeros((experts * capacity,), jnp.int32)
        .at[slots]
        .set(jnp.arange(top * count, dtype=jnp.int32) // top)
    )
    values = tokens.astype(jnp.float32)
    squares = lax.psum(jnp.sum(values * values, axis=1), "tp")
    width = tokens.shape[1] * lax.axis_size("tp")
    normed = (values * lax.rsqrt(squares / width + 1e-06)[:, None]).astype(jnp.bfloat16)
    outbound = normed[owners].reshape(experts, capacity, tokens.shape[1])
    arrived = lax.all_to_all(outbound, "fs", split_axis=0, concat_axis=0, tiled=True).reshape(
        -1, tokens.shape[1]
    )
    piece = lax.all_gather(arrived, "tp", axis=1, tiled=True)
    gate = jnp.dot(piece, gate_local[0], preferred_element_type=jnp.float32)
    up = jnp.dot(piece, up_local[0], preferred_element_type=jnp.float32)
    hidden = (jax.nn.silu(gate) * up).astype(jnp.bfloat16)
    partial_value = jnp.dot(hidden, down_local[0], preferred_element_type=jnp.float32).astype(
        jnp.bfloat16
    )
    row_count = partial_value.shape[0]
    tp_count = lax.axis_size("tp")
    split_blocks = partial_value.reshape(row_count, tp_count, partial_value.shape[1] // tp_count)
    received = lax.all_to_all(split_blocks, "tp", split_axis=1, concat_axis=1, tiled=True)
    summed = jnp.sum(received.astype(jnp.float32), axis=1).astype(jnp.bfloat16)
    columns = summed.shape[1]
    returned = lax.all_to_all(
        summed.reshape(experts, capacity, columns), "fs", split_axis=0, concat_axis=0, tiled=True
    )
    picked = (
        returned.reshape(experts * capacity, columns)[slots]
        .astype(jnp.float32)
        .reshape(count, top, columns)
    )
    mixed = jnp.sum(picked * route_weights[:, :, None], axis=1).astype(jnp.bfloat16)
    return (gate_local, up_local, down_local, mixed)


def solution(mesh):
    placed = (
        P(("grp", "fs"), "tp"),
        P("fs"),
        P(None, "fs", "tp"),
        P(None, "fs", "tp"),
        P(None, "fs", "tp"),
        P(("grp", "fs"), None),
        P(("grp", "fs"), None),
    )
    sizes = mesh.shape
    square = sizes["fs"] == sizes["tp"] and sizes["grp"] == 2 and sizes["fs"] % 2 == 0
    return jax.shard_map(
        quick if square else plain,
        mesh=mesh,
        in_specs=placed,
        out_specs=(
            P(("grp", "fs"), None, "tp"),
            P(("grp", "fs"), None, "tp"),
            P(("grp", "fs"), "tp", None),
            P(("grp", "fs"), "tp"),
        ),
        check_vma=False,
    )
```
